32 devices in a mesh: sp: 16 (over z, y, core), tp: 2 (over x).
Axes of the slice: x: 2, y: 2, z: 4, core: 2. Of those that a mesh axis runs over, the one named last changes fastest.
Arguments:
- stream: bfloat16 [16384, 2048], P('sp'), may hold values from -6 to 6
- queries: bfloat16 [16384, 1024], P('sp', 'tp'), may hold values from -6 to 6
- projected_keys: bfloat16 [16384, 1024], P('sp', 'tp'), may hold values from -6 to 6
- values: bfloat16 [16384, 2048], P('sp', 'tp'), may hold values from -6 to 6
- decay_gate_logits: bfloat16 [16384, 1024], P('sp', 'tp'), may hold values from -7 to 7
- decay_gate_bias: float32 [1024], P('tp')
- extra_log_decay: float32 [16384, 8], P('sp', 'tp'), may hold values from -0.7 to 0
- document_index: int32 [16384], P('sp'), may hold values from 0 to 3, never falling along the last dimension, each value on 1 to 8192 neighbouring positions
- output_gate: bfloat16 [16384, 2048], P('sp', 'tp'), may hold values from -6 to 6
- head_norm_gain: bfloat16 [256], replicated, may hold values from 0.099609375 to 1.8984375
- output_weight: bfloat16 [2048, 2048], P('tp'), may hold values from -0.125 to 0.125
- feedforward_norm_gain: bfloat16 [2048], replicated, may hold values from 0.099609375 to 1.8984375
- gate_weight: bfloat16 [2048, 5632], P('sp', 'tp'), may hold values from -0.125 to 0.125
- up_weight: bfloat16 [2048, 5632], P('sp', 'tp'), may hold values from -0.125 to 0.125
- down_weight: bfloat16 [5632, 2048], P('tp', 'sp'), may hold values from -0.078125 to 0.078125
Outputs:
- updated: bfloat16 [16384, 2048], P(('sp', 'tp'))
The draws below stay inside these ranges and needn't reach their ends.
All inputs are finite; a program needn't handle non-finite values.
Results may differ from the reference program's by a relative error of at most 0.015.
Values may be sent and summed in bfloat16 or wider, within the bound.
No kernel may reach another device: no remote copies, remote signals or barrier semaphores. Data moves between devices by JAX's collectives and lax.ppermute only.
A program may use at most 128 MiB of HBM per device.

```python
import math
import jax
import jax.numpy as jnp
import numpy as np
from jax import lax

D = 2048
FF = 5632
HEAD_TOTAL = 8
DK = 128
DV = 256
BLOCK_LENGTH = 64
TOK_DEV = 1024
TOKENS = 16384
QK = 1024
VDIM = 2048
N_SP = 16
N_TP = 2


def draw_decay_gate_logits(key, part):
    noise_key, shift_key = jax.random.split(jax.random.fold_in(key, 11))
    blocks = TOKENS // TOK_DEV
    block_shift = jax.random.uniform(shift_key, (blocks, 1, 1), jnp.float32, -0.7, 0.7)
    noise_part = jnp.clip(jax.random.normal(noise_key, (blocks, TOK_DEV, QK), jnp.float32), -6.0, 6.0)
    return (noise_part + block_shift).reshape(TOKENS, QK).astype(jnp.bfloat16)


def draw_decay_gate_bias(key, part):
    slow_key, fast_key, level_key = jax.random.split(jax.random.fold_in(key, 23), 3)
    slow_heads = jax.random.uniform(slow_key, (HEAD_TOTAL,), jnp.float32) < 0.5
    base_level = jnp.log(jnp.float32(TOKENS)) - 2.0
    slow_level = base_level + jax.random.uniform(level_key, (HEAD_TOTAL, DK), jnp.float32, 0.0, 2.0)
    fast_level = jax.random.uniform(fast_key, (HEAD_TOTAL, DK), jnp.float32, 0.0, 1.0)
    return jnp.where(slow_heads[:, None], slow_level, fast_level).reshape(HEAD_TOTAL * DK)


def draw_extra_log_decay(key, part):
    place_key, size_random_key = jax.random.split(jax.random.fold_in(key, 37))
    head_keys = jax.random.split(place_key, HEAD_TOTAL)
    orders = jax.vmap(lambda single: jax.random.permutation(single, TOKENS))(head_keys)
    places = jnp.transpose(orders[:, :3])
    extra_decay_sizes = jnp.log(jax.random.uniform(size_random_key, (3, HEAD_TOTAL), jnp.float32, 0.5, 0.8))
    positions = jnp.arange(TOKENS)[:, None, None]
    matched_positions = (positions == places[None]).astype(jnp.float32)
    return jnp.sum(matched_positions * extra_decay_sizes[None], axis=1)


def steps_of(stream_key, dims, cuts, smallest, high):
    def one(dim, blocks):
        draws = jax.random.uniform(jax.random.fold_in(jax.random.fold_in(stream_key, 6), dim), (blocks,), jnp.float32, smallest / len(cuts), high / len(cuts))
        return jnp.repeat(jnp.exp(draws), dims[dim] // blocks).reshape((-1,) + (1,) * (len(dims) - dim - 1))

    level = one(*cuts[0])
    for cut in cuts[1:]:
        level = level * one(*cut)
    return level


def split_up(number_of, total, reach, slope):
    loads = [(1 << 20) // math.isqrt(rank ** slope) + 1 for rank in range(2, number_of + 1)]
    spare, given = total - reach - (number_of - 1), [1] * (number_of - 1)
    while spare > 0:
        free = [i for i in range(number_of - 1) if given[i] < reach]
        whole, budget = sum([loads[i] for i in free]), spare
        for i in free:
            addition = min(reach - given[i], max(1, budget * loads[i] // whole), spare)
            given[i] = given[i] + addition
            spare = spare - addition
    return np.array([reach] + given)


def uneven_parts(stream_key, number_of, total, most, skew):
    if number_of == 2:
        one = jax.random.randint(stream_key, (), max(1, total - most), min(most, total - 1) + 1)
        return jnp.stack([one, total - one])
    lengths = jnp.asarray(split_up(number_of, total, most, skew), jnp.int32)
    couples = (number_of - 1) // 2
    giver, receiver = lengths[1:1 + 2 * couples:2], lengths[2:2 + 2 * couples:2]
    margin = jnp.minimum(giver - 1, most - receiver)
    passed = jax.random.randint(jax.random.fold_in(stream_key, 1), (couples,), 0, 1 << 20) % (margin + 1)
    lengths = lengths.at[1:1 + 2 * couples:2].set(giver - passed).at[2:2 + 2 * couples:2].set(receiver + passed)
    return lengths[jax.random.permutation(jax.random.fold_in(stream_key, 2), number_of)]


def gaussian(rng, dims, spread, reach, shards=(), kind=jnp.bfloat16):
    values = jax.random.normal(rng, dims, jnp.float32) * spread
    if len(shards) > 0:
        values = steps_of(rng, dims, shards, -0.22, 0.18) * values
    return jnp.clip(values, min=-reach, max=reach).astype(kind)


def setup_inputs(seed: int = 0) -> dict:
    splits = jax.random.split(jax.random.key(seed), 16)
    stream = gaussian(splits[0], (TOKENS, D), 1.0, 6.0, ((0, 16),))
    queries = gaussian(splits[1], (TOKENS, QK), 1.0, 6.0, ((0, 16), (1, 2)))
    projected_keys = gaussian(splits[2], (TOKENS, QK), 1.0, 6.0, ((0, 16), (1, 2)))
    values = gaussian(splits[3], (TOKENS, VDIM), 1.0, 6.0, ((0, 16), (1, 2)))
    decay_gate_logits = draw_decay_gate_logits(jax.random.fold_in(splits[15], 71), 0)
    decay_gate_bias = draw_decay_gate_bias(jax.random.fold_in(splits[15], 71), 0)
    extra_log_decay = draw_extra_log_decay(jax.random.fold_in(splits[15], 71), 0)
    document_index = jnp.searchsorted(jnp.cumsum(uneven_parts(splits[7], N_SP // 4, TOKENS, TOKENS // 2, 0)), jnp.arange(TOKENS), side="right").astype(jnp.int32)
    output_gate = gaussian(splits[8], (TOKENS, VDIM), 1.0, 6.0, ((0, 16), (1, 2)))
    head_norm_gain = jnp.clip(1.0 + 0.18 * jax.random.normal(splits[9], (DV,), jnp.float32), 0.099609375, 1.8984375).astype(jnp.bfloat16)
    output_weight = gaussian(splits[10], (VDIM, D), VDIM ** -0.5, 0.125, ((0, 2),))
    feedforward_norm_gain = jnp.clip(1.0 + 0.18 * jax.random.normal(splits[11], (D,), jnp.float32), 0.099609375, 1.8984375).astype(jnp.bfloat16)
    gate_weight = gaussian(splits[12], (D, FF), D ** -0.5, 0.125, ((0, 16), (1, 2)))
    up_weight = gaussian(splits[13], (D, FF), D ** -0.5, 0.125, ((0, 16), (1, 2)))
    down_weight = gaussian(splits[14], (FF, D), FF ** -0.5, 0.078125, ((0, 2), (1, 16)))
    return {"stream": stream, "queries": queries, "projected_keys": projected_keys, "values": values, "decay_gate_logits": decay_gate_logits, "decay_gate_bias": decay_gate_bias, "extra_log_decay": extra_log_decay, "document_index": document_index, "output_gate": output_gate, "head_norm_gain": head_norm_gain, "output_weight": output_weight, "feedforward_norm_gain": feedforward_norm_gain, "gate_weight": gate_weight, "up_weight": up_weight, "down_weight": down_weight}


TAU = 16.0
EPS = 1e-06
HIGH = lax.Precision.HIGHEST

def combine(earlier, later):
    decay_e, state_e, entry_e, exit_e = earlier
    decay_l, state_l, entry_l, exit_l = later
    joined = (exit_e == entry_l) | (exit_e < 0.0) | (entry_l < 0.0)
    passing = decay_l * joined.astype(decay_l.dtype)[..., None, None]
    merged_state = state_l + passing[..., None] * state_e
    merged_decay = decay_e * passing
    entry_doc = jnp.where(entry_e < 0.0, entry_l, entry_e)
    exit_doc = jnp.where(exit_l < 0.0, exit_e, exit_l)
    return (merged_decay, merged_state, entry_doc, exit_doc)

def neutral(head_number, key_channels, val_dim):
    return (jnp.ones((head_number, key_channels), jnp.float32), jnp.zeros((head_number, key_channels, val_dim), jnp.float32), jnp.full((), -1.0, jnp.float32), jnp.full((), -1.0, jnp.float32))

def block_prefix(elements, initial, reverse_dir):

    def advance(running, element):
        return (combine(running, element), running)
    totals, before = lax.scan(advance, initial, elements, reverse=reverse_dir)
    return (before, totals)

def attention_variant(queries, projected_keys, values, decay_gate_logits, decay_gate_bias, extra_log_decay, document_index, block_length):
    head_number = extra_log_decay.shape[1]
    row_number = queries.shape[0]
    blocks = row_number // block_length
    key_channels = queries.shape[1] // head_number
    val_dim = values.shape[1] // head_number
    query_f = queries.astype(jnp.float32).reshape(blocks, block_length, head_number, key_channels) * key_channels ** (-0.5)
    key_f = projected_keys.astype(jnp.float32).reshape(blocks, block_length, head_number, key_channels)
    value_b = values.reshape(blocks, block_length, head_number, val_dim)
    decay_logarithm = jax.nn.log_sigmoid(decay_gate_logits.astype(jnp.float32) + decay_gate_bias) / TAU
    decay_logarithm = decay_logarithm.reshape(row_number, head_number, key_channels) + extra_log_decay[:, :, None]
    cumulative = jnp.cumsum(decay_logarithm.reshape(blocks, block_length, head_number, key_channels), axis=1)
    document_float = document_index.astype(jnp.float32).reshape(blocks, block_length)
    middle = cumulative[:, block_length // 2 - 1:block_length // 2]
    rising = jnp.exp(cumulative - middle)
    falling = jnp.exp(middle - cumulative)
    forward = jnp.einsum('bihc,bjhc->bhij', (query_f * rising).astype(jnp.bfloat16), (key_f * falling).astype(jnp.bfloat16), preferred_element_type=jnp.float32)
    backward = jnp.einsum('bihc,bjhc->bhij', (query_f * falling).astype(jnp.bfloat16), (key_f * rising).astype(jnp.bfloat16), preferred_element_type=jnp.float32)
    offsets = jnp.arange(block_length)
    same_doc = (document_float[:, :, None] == document_float[:, None, :])[:, None]
    below_mask = offsets[None, :] <= offsets[:, None]
    above_mask = offsets[None, :] >= offsets[:, None]
    scores = jnp.where(same_doc & below_mask, forward, 0.0) + jnp.where(same_doc & above_mask, backward, 0.0)
    within_block = jnp.einsum('bhij,bjhv->bihv', scores.astype(jnp.bfloat16), value_b, preferred_element_type=jnp.float32)
    block_end = cumulative[:, block_length - 1]
    first_doc = document_float[:, 0]
    last_doc = document_float[:, block_length - 1]
    through = jnp.exp(block_end) * (first_doc == last_doc).astype(jnp.float32)[:, None, None]
    tail_mask = (document_float == last_doc[:, None]).astype(jnp.float32)[:, :, None, None]
    head_mask = (document_float == first_doc[:, None]).astype(jnp.float32)[:, :, None, None]
    tail_keys = (key_f * jnp.exp(block_end[:, None] - cumulative) * tail_mask).astype(jnp.bfloat16)
    head_keys = (key_f * jnp.exp(cumulative) * head_mask).astype(jnp.bfloat16)
    fwd_state = jnp.einsum('bjhc,bjhv->bhcv', tail_keys, value_b, preferred_element_type=jnp.float32)
    bwd_state = jnp.einsum('bjhc,bjhv->bhcv', head_keys, value_b, preferred_element_type=jnp.float32)
    forward_elements = (through, fwd_state, first_doc, last_doc)
    backward_elements = (through, bwd_state, last_doc, first_doc)
    forward_query = query_f * jnp.exp(cumulative)
    backward_query = query_f * jnp.exp(block_end[:, None] - cumulative)
    return (within_block, forward_elements, backward_elements, forward_query, backward_query, document_float)

def carried(inflow, factor, document_float):
    hit_mask = (document_float == inflow[3][:, None]).astype(jnp.float32)[:, :, None, None]
    return jnp.einsum('bihc,bhcv->bihv', factor, inflow[1], precision=HIGH) * hit_mask

def head_mix(within_block, fwd_in, bwd_in, forward_query, backward_query, document_float, output_gate, head_norm_gain, head_number):
    total_out = within_block + carried(fwd_in, forward_query, document_float) + carried(bwd_in, backward_query, document_float)
    row_number = output_gate.shape[0]
    total_out = total_out.reshape(row_number, head_number, -1)
    scaled = total_out * lax.rsqrt(lax.optimization_barrier(jnp.mean(total_out * total_out, axis=-1, keepdims=True)) + EPS)
    scaled = scaled * head_norm_gain.astype(jnp.float32)
    return (scaled.reshape(row_number, -1) * jax.nn.silu(output_gate.astype(jnp.float32))).astype(jnp.bfloat16)

def row_norm(rows_f, gain):
    factor = lax.rsqrt(lax.optimization_barrier(jnp.mean(rows_f * rows_f, axis=-1, keepdims=True)) + EPS)
    return (rows_f * factor * gain.astype(jnp.float32)).astype(jnp.bfloat16)

def reference(stream, queries, projected_keys, values, decay_gate_logits, decay_gate_bias, extra_log_decay, document_index, output_gate, head_norm_gain, output_weight, feedforward_norm_gain, gate_weight, up_weight, down_weight):
    head_number = extra_log_decay.shape[1]
    key_channels = queries.shape[1] // head_number
    val_dim = values.shape[1] // head_number
    within_block, forward_elements, backward_elements, forward_query, backward_query, document_float = attention_variant(queries, projected_keys, values, decay_gate_logits, decay_gate_bias, extra_log_decay, document_index, BLOCK_LENGTH)
    initial = neutral(head_number, key_channels, val_dim)
    fwd_in = block_prefix(forward_elements, initial, False)[0]
    bwd_in = block_prefix(backward_elements, initial, True)[0]
    head_mixed = head_mix(within_block, fwd_in, bwd_in, forward_query, backward_query, document_float, output_gate, head_norm_gain, head_number)
    col_group = values.shape[1] // N_TP
    attended = jnp.zeros(stream.shape, jnp.float32)
    for group_idx in range(N_TP):
        lower_col = group_idx * col_group
        partial_value = jnp.dot(head_mixed[:, lower_col:lower_col + col_group], output_weight[lower_col:lower_col + col_group], preferred_element_type=jnp.float32)
        attended = attended + lax.optimization_barrier(partial_value.astype(jnp.bfloat16)).astype(jnp.float32)
    resid = stream.astype(jnp.float32) + attended
    normed = row_norm(resid, feedforward_norm_gain)
    unit_group = gate_weight.shape[1] // N_TP
    mlp_out = jnp.zeros(stream.shape, jnp.float32)
    for group_idx in range(N_TP):
        lower_unit = group_idx * unit_group
        gate_act = jnp.dot(normed, gate_weight[:, lower_unit:lower_unit + unit_group], preferred_element_type=jnp.float32)
        up_act = jnp.dot(normed, up_weight[:, lower_unit:lower_unit + unit_group], preferred_element_type=jnp.float32)
        hidden = (jax.nn.silu(gate_act) * up_act).astype(jnp.bfloat16)
        partial_value = jnp.dot(hidden, down_weight[lower_unit:lower_unit + unit_group], preferred_element_type=jnp.float32)
        mlp_out = mlp_out + lax.optimization_barrier(partial_value.astype(jnp.bfloat16)).astype(jnp.float32)
    return (resid + mlp_out).astype(jnp.bfloat16)
```

```python
import jax
import jax.numpy as jnp
from jax import lax
from jax.experimental import pallas as pl
from jax.experimental.pallas import tpu as pltpu
from jax.sharding import PartitionSpec as P

BLOCK_LENGTH = 64
TAU = 16.0
EPS = 1e-06
F32 = jnp.float32
BF = jnp.bfloat16


def nt(a, b):
    return lax.dot_general(a, b, (((1,), (1,)), ((), ())), preferred_element_type=F32)


def tn(a, b):
    return lax.dot_general(a, b, (((0,), (0,)), ((), ())), preferred_element_type=F32)


def local_kernel(
    q_ref, k_ref, v_ref, g_ref, bias_ref, extra_ref, doc_ref, docrow_ref,
    o_ref, qc_ref, state_f_ref, state_b_ref, log_ref, back_ref, cum_ref,
):
    L = BLOCK_LENGTH
    rows, dk = q_ref.shape
    heads = extra_ref.shape[1]
    blocks = rows // L
    h = pl.program_id(0)
    pick = lax.broadcasted_iota(jnp.int32, (L, heads), 1) == h
    r = lax.broadcasted_iota(jnp.int32, (L, L), 0)
    c = lax.broadcasted_iota(jnp.int32, (L, L), 1)
    tril = (c <= r).astype(F32)
    scale = dk ** (-0.5)
    docs = [docrow_ref[b : b + 1, :] for b in range(blocks)]
    firsts = [d[:, 0:1] for d in docs]
    lasts = [d[:, L - 1 : L] for d in docs]
    running = None
    logs = jnp.zeros((1, dk), F32)
    ends = []
    for b in range(blocks):
        rs = pl.ds(b * L, L)
        gate = g_ref[rs, :].astype(F32) + bias_ref[...]
        logsig = jnp.minimum(gate, 0.0) - jnp.log1p(jnp.exp(-jnp.abs(gate)))
        extra = jnp.sum(jnp.where(pick, extra_ref[rs, :], 0.0), axis=1, keepdims=True)
        decay = logsig / TAU + extra
        cum = jnp.dot(tril, decay, precision=lax.Precision.HIGHEST, preferred_element_type=F32)
        cum_ref[rs, :] = cum
        mid = cum[L // 2 - 1 : L // 2]
        end = cum[L - 1 : L]
        ends.append(end)
        q = q_ref[rs, :].astype(F32) * scale
        k = k_ref[rs, :].astype(F32)
        v = v_ref[rs, :]
        up = jnp.exp(cum - mid)
        down = jnp.exp(mid - cum)
        fwd = nt((q * up).astype(BF), (k * down).astype(BF))
        bwd = nt((q * down).astype(BF), (k * up).astype(BF))
        col = doc_ref[rs, :]
        same = col == docs[b]
        scores = jnp.where(same & (c <= r), fwd, 0.0) + jnp.where(same & (c >= r), bwd, 0.0)
        out = jnp.dot(scores.astype(BF), v, preferred_element_type=F32)
        tail = (k * jnp.exp(end - cum) * (col == lasts[b]).astype(F32)).astype(BF)
        head = (k * jnp.exp(cum) * (col == firsts[b]).astype(F32)).astype(BF)
        state = tn(v, tail)
        back_ref[b] = tn(v, head)
        qf = q * jnp.exp(cum)
        if b > 0:
            hit = (col == lasts[b - 1]).astype(F32)
            out = out + nt((qf * hit).astype(BF), running.astype(BF))
            running = state + (jnp.exp(end) * (lasts[b] == lasts[b - 1]).astype(F32)) * running
        else:
            running = state
        o_ref[rs, :] = out
        qc_ref[rs, 0:dk] = (qf * jnp.exp(logs)).astype(BF)
        logs = logs + end
    state_f_ref[0] = running
    log_ref[0] = logs
    logs = jnp.zeros((1, dk), F32)
    for b in reversed(range(blocks)):
        rs = pl.ds(b * L, L)
        q = q_ref[rs, :].astype(F32) * scale
        qb = q * jnp.exp(ends[b] - cum_ref[rs, :])
        state = back_ref[b]
        if b < blocks - 1:
            hit = (doc_ref[rs, :] == firsts[b + 1]).astype(F32)
            o_ref[rs, :] += nt((qb * hit).astype(BF), running.astype(BF))
            passing = jnp.exp(ends[b]) * (firsts[b] == firsts[b + 1]).astype(F32)
            running = state + passing * running
        else:
            running = state
        qc_ref[rs, dk : 2 * dk] = (qb * jnp.exp(logs)).astype(BF)
        logs = logs + ends[b]
    state_b_ref[0] = running


def local_attention(q, k, v, g, bias, extra, docs):
    rows, heads = extra.shape
    dk, dv = q.shape[1] // heads, v.shape[1] // heads
    blocks = rows // BLOCK_LENGTH
    docf = docs.astype(F32)

    def lanes(width):
        return pl.BlockSpec((rows, width), lambda h: (0, h))

    def whole(shape):
        return pl.BlockSpec(shape, lambda h: (0, 0))

    per_head = pl.BlockSpec((1, dv, dk), lambda h: (h, 0, 0))
    return pl.pallas_call(
        local_kernel,
        grid=(heads,),
        in_specs=[
            lanes(dk), lanes(dk), lanes(dv), lanes(dk),
            pl.BlockSpec((1, dk), lambda h: (0, h)),
            whole((rows, heads)), whole((rows, 1)), whole((blocks, BLOCK_LENGTH)),
        ],
        out_specs=[
            lanes(dv), lanes(2 * dk), per_head, per_head,
            pl.BlockSpec((1, 1, dk), lambda h: (h, 0, 0)),
        ],
        out_shape=[
            jax.ShapeDtypeStruct((rows, heads * dv), F32),
            jax.ShapeDtypeStruct((rows, heads * 2 * dk), BF),
            jax.ShapeDtypeStruct((heads, dv, dk), F32),
            jax.ShapeDtypeStruct((heads, dv, dk), F32),
            jax.ShapeDtypeStruct((heads, 1, dk), F32),
        ],
        scratch_shapes=[pltpu.VMEM((blocks, dv, dk), F32), pltpu.VMEM((rows, dk), F32)],
        cost_estimate=pl.CostEstimate(
            flops=60_000_000_000, bytes_accessed=20_000_000, transcendentals=0
        ),
        name="local_attention",
    )(q, k, v, g, bias.reshape(1, -1), extra, docf.reshape(rows, 1),
      docf.reshape(blocks, BLOCK_LENGTH))


def mix_kernel(o_ref, qc_ref, cf_ref, cb_ref, doc_ref, edge_ref, gate_ref, gain_ref, out_ref):
    dk = cf_ref.shape[2]
    doc = doc_ref[...]
    qf = qc_ref[:, 0:dk]
    qb = qc_ref[:, dk : 2 * dk]
    total = o_ref[...]
    total = total + nt(qf, cf_ref[0]) * (doc == edge_ref[:, 0:1]).astype(F32)
    total = total + nt(qb, cb_ref[0]) * (doc == edge_ref[:, 1:2]).astype(F32)
    scaled = total * lax.rsqrt(jnp.mean(total * total, axis=-1, keepdims=True) + EPS)
    gate = gate_ref[...].astype(F32)
    act = gate / (1.0 + jnp.exp(-gate))
    out_ref[...] = (scaled * gain_ref[...].astype(F32) * act).astype(BF)


def head_mix(o, qc, cf, cb, docs, edges, gate, gain):
    rows = o.shape[0]
    heads, dv, dk = cf.shape
    tile = rows // 4
    per_head = pl.BlockSpec((1, dv, dk), lambda h, i: (h, 0, 0))
    return pl.pallas_call(
        mix_kernel,
        grid=(heads, 4),
        in_specs=[
            pl.BlockSpec((tile, dv), lambda h, i: (i, h)),
            pl.BlockSpec((tile, 2 * dk), lambda h, i: (i, h)),
            per_head, per_head,
            pl.BlockSpec((tile, 1), lambda h, i: (i, 0)),
            pl.BlockSpec((1, 2), lambda h, i: (0, 0)),
            pl.BlockSpec((tile, dv), lambda h, i: (i, h)),
            pl.BlockSpec((1, dv), lambda h, i: (0, 0)),
        ],
        out_specs=pl.BlockSpec((tile, dv), lambda h, i: (i, h)),
        out_shape=jax.ShapeDtypeStruct((rows, heads * dv), BF),
        cost_estimate=pl.CostEstimate(
            flops=5_000_000_000, bytes_accessed=12_000_000, transcendentals=0
        ),
        name="head_mix",
    )(o, qc, cf, cb, docs.astype(F32).reshape(rows, 1), edges, gate, gain.reshape(1, -1))


def shift(x, axis, by):
    n = lax.axis_size(axis)
    return lax.ppermute(x, axis, [(i, i + by) for i in range(n) if 0 <= i + by < n])


def rotate(x, axis, by):
    n = lax.axis_size(axis)
    return lax.ppermute(x, axis, [(i, (i + by) % n) for i in range(n)])


def carry_scan(states, decays, axis, signs):
    n = lax.axis_size(axis)

    def sent(s, a, by):
        return (shift(s.astype(BF), axis, by).astype(F32), shift(a, axis, by))

    pairs = [sent(s, a, g) for s, a, g in zip(states, decays, signs)]
    step = 1
    while step < n - 1:
        moved = [sent(s, a, g * step) for (s, a), g in zip(pairs, signs)]
        pairs = [(s + a * ms, a * ma) for (s, a), (ms, ma) in zip(pairs, moved)]
        step *= 2
    return [s.astype(BF) for s, _ in pairs]


def row_norm(rows_f, gain):
    factor = lax.rsqrt(jnp.mean(rows_f * rows_f, axis=-1, keepdims=True) + EPS)
    return (rows_f * factor * gain.astype(F32)).astype(BF)


def dot(a, b):
    return jnp.dot(a, b, preferred_element_type=F32)


def per_device(
    stream, queries, projected_keys, values, decay_gate_logits, decay_gate_bias,
    extra_log_decay, document_index, output_gate, head_norm_gain, output_weight,
    feedforward_norm_gain, gate_weight, up_weight, down_weight,
):
    gate_all = lax.all_gather(gate_weight, "sp", axis=0, tiled=True)
    up_all = lax.all_gather(up_weight, "sp", axis=0, tiled=True)
    down_all = lax.all_gather(down_weight, "sp", axis=1, tiled=True)
    docf = document_index.astype(F32)
    first, last = docf[:1], docf[-1:]
    prev_last = shift(last + 1.0, "sp", 1) - 1.0
    next_first = shift(first + 1.0, "sp", -1) - 1.0
    o, qc, sf, sb, logs = local_attention(
        queries, projected_keys, values, decay_gate_logits, decay_gate_bias,
        extra_log_decay, document_index,
    )
    decay = jnp.exp(logs)
    cf, cb = carry_scan(
        (sf, sb),
        (decay * (last == prev_last).astype(F32), decay * (first == next_first).astype(F32)),
        "sp",
        (1, -1),
    )
    edges = jnp.concatenate([prev_last, next_first]).reshape(1, 2)
    mixed = head_mix(o, qc, cf, cb, document_index, edges, output_gate, head_norm_gain)
    n = lax.axis_size("tp")
    me = lax.axis_index("tp")
    rows = stream.shape[0] // n

    def chunk(x, s):
        return lax.dynamic_slice_in_dim(x, (me + s) % n * rows, rows, 0)

    pieces = []
    for s in range(1, n):
        part = dot(chunk(mixed, s), output_weight).astype(BF)
        pieces.append(rotate(part, "tp", s))
    attended = dot(chunk(mixed, 0), output_weight).astype(BF).astype(F32)
    for piece in pieces:
        attended = attended + piece.astype(F32)
    resid = chunk(stream, 0).astype(F32) + attended
    normed = row_norm(resid, feedforward_norm_gain)
    others = [rotate(normed, "tp", s) for s in range(1, n)]

    def feed(x):
        hidden = (jax.nn.silu(dot(x, gate_all)) * dot(x, up_all)).astype(BF)
        return dot(hidden, down_all).astype(BF)

    returned = [rotate(feed(x), "tp", -s) for s, x in enumerate(others, 1)]
    mlp_out = feed(normed).astype(F32)
    for piece in returned:
        mlp_out = mlp_out + piece.astype(F32)
    return (resid + mlp_out).astype(BF)


def solution(mesh):
    placed = (
        P("sp", None), P("sp", "tp"), P("sp", "tp"), P("sp", "tp"), P("sp", "tp"), P("tp"),
        P("sp", "tp"), P("sp"), P("sp", "tp"), P(), P("tp", None), P(), P("sp", "tp"),
        P("sp", "tp"), P("tp", "sp"),
    )
    return jax.shard_map(
        per_device, mesh=mesh, in_specs=placed, out_specs=P(("sp", "tp"), None), check_vma=False
    )
```

```python
import jax
import jax.numpy as jnp
from jax import lax
from jax.experimental import pallas as pl
from jax.experimental.pallas import tpu as pltpu
from jax.sharding import PartitionSpec as P

BLOCK_LENGTH = 64
TAU = 16.0
EPS = 1e-06
F32 = jnp.float32
BF = jnp.bfloat16


def nt(a, b):
    return lax.dot_general(a, b, (((1,), (1,)), ((), ())), preferred_element_type=F32)


def tn(a, b):
    return lax.dot_general(a, b, (((0,), (0,)), ((), ())), preferred_element_type=F32)


def local_kernel(
    q_ref, k_ref, v_ref, g_ref, bias_ref, extra_ref, doc_ref, docrow_ref,
    o_ref, qc_ref, state_f_ref, state_b_ref, log_ref, back_ref, cum_ref,
):
    L = BLOCK_LENGTH
    rows, dk = q_ref.shape
    heads = extra_ref.shape[1]
    blocks = rows // L
    h = pl.program_id(0)
    pick = lax.broadcasted_iota(jnp.int32, (L, heads), 1) == h
    r = lax.broadcasted_iota(jnp.int32, (L, L), 0)
    c = lax.broadcasted_iota(jnp.int32, (L, L), 1)
    tril = (c <= r).astype(F32)
    scale = dk ** (-0.5)
    docs = [docrow_ref[b : b + 1, :] for b in range(blocks)]
    firsts = [d[:, 0:1] for d in docs]
    lasts = [d[:, L - 1 : L] for d in docs]
    running = None
    logs = jnp.zeros((1, dk), F32)
    ends = []
    for b in range(blocks):
        rs = pl.ds(b * L, L)
        gate = g_ref[rs, :].astype(F32) + bias_ref[...]
        logsig = jnp.minimum(gate, 0.0) - jnp.log1p(jnp.exp(-jnp.abs(gate)))
        extra = jnp.sum(jnp.where(pick, extra_ref[rs, :], 0.0), axis=1, keepdims=True)
        decay = logsig / TAU + extra
        cum = jnp.dot(tril, decay, precision=lax.Precision.HIGHEST, preferred_element_type=F32)
        cum_ref[rs, :] = cum
        mid = cum[L // 2 - 1 : L // 2]
        end = cum[L - 1 : L]
        ends.append(end)
        q = q_ref[rs, :].astype(F32) * scale
        k = k_ref[rs, :].astype(F32)
        v = v_ref[rs, :]
        up = jnp.exp(cum - mid)
        down = jnp.exp(mid - cum)
        fwd = nt((q * up).astype(BF), (k * down).astype(BF))
        bwd = nt((q * down).astype(BF), (k * up).astype(BF))
        col = doc_ref[rs, :]
        same = col == docs[b]
        scores = jnp.where(same & (c <= r), fwd, 0.0) + jnp.where(same & (c >= r), bwd, 0.0)
        out = jnp.dot(scores.astype(BF), v, preferred_element_type=F32)
        tail = (k * jnp.exp(end - cum) * (col == lasts[b]).astype(F32)).astype(BF)
        head = (k * jnp.exp(cum) * (col == firsts[b]).astype(F32)).astype(BF)
        state = tn(v, tail)
        back_ref[b] = tn(v, head)
        qf = q * jnp.exp(cum)
        if b > 0:
            hit = (col == lasts[b - 1]).astype(F32)
            out = out + nt((qf * hit).astype(BF), running.astype(BF))
            running = state + (jnp.exp(end) * (lasts[b] == lasts[b - 1]).astype(F32)) * running
        else:
            running = state
        o_ref[rs, :] = out
        qc_ref[rs, 0:dk] = (qf * jnp.exp(logs)).astype(BF)
        logs = logs + end
    state_f_ref[0] = running
    log_ref[0] = logs
    logs = jnp.zeros((1, dk), F32)
    for b in reversed(range(blocks)):
        rs = pl.ds(b * L, L)
        q = q_ref[rs, :].astype(F32) * scale
        qb = q * jnp.exp(ends[b] - cum_ref[rs, :])
        state = back_ref[b]
        if b < blocks - 1:
            hit = (doc_ref[rs, :] == firsts[b + 1]).astype(F32)
            o_ref[rs, :] += nt((qb * hit).astype(BF), running.astype(BF))
            passing = jnp.exp(ends[b]) * (firsts[b] == firsts[b + 1]).astype(F32)
            running = state + passing * running
        else:
            running = state
        qc_ref[rs, dk : 2 * dk] = (qb * jnp.exp(logs)).astype(BF)
        logs = logs + ends[b]
    state_b_ref[0] = running


def local_attention(q, k, v, g, bias, extra, docs):
    rows, heads = extra.shape
    dk, dv = q.shape[1] // heads, v.shape[1] // heads
    blocks = rows // BLOCK_LENGTH
    docf = docs.astype(F32)

    def lanes(width):
        return pl.BlockSpec((rows, width), lambda h: (0, h))

    def whole(shape):
        return pl.BlockSpec(shape, lambda h: (0, 0))

    per_head = pl.BlockSpec((1, dv, dk), lambda h: (h, 0, 0))
    return pl.pallas_call(
        local_kernel,
        grid=(heads,),
        in_specs=[
            lanes(dk), lanes(dk), lanes(dv), lanes(dk),
            pl.BlockSpec((1, dk), lambda h: (0, h)),
            whole((rows, heads)), whole((rows, 1)), whole((blocks, BLOCK_LENGTH)),
        ],
        out_specs=[
            lanes(dv), lanes(2 * dk), per_head, per_head,
            pl.BlockSpec((1, 1, dk), lambda h: (h, 0, 0)),
        ],
        out_shape=[
            jax.ShapeDtypeStruct((rows, heads * dv), F32),
            jax.ShapeDtypeStruct((rows, heads * 2 * dk), BF),
            jax.ShapeDtypeStruct((heads, dv, dk), F32),
            jax.ShapeDtypeStruct((heads, dv, dk), F32),
            jax.ShapeDtypeStruct((heads, 1, dk), F32),
        ],
        scratch_shapes=[pltpu.VMEM((blocks, dv, dk), F32), pltpu.VMEM((rows, dk), F32)],
        cost_estimate=pl.CostEstimate(
            flops=60_000_000_000, bytes_accessed=20_000_000, transcendentals=0
        ),
        name="local_attention",
    )(q, k, v, g, bias.reshape(1, -1), extra, docf.reshape(rows, 1),
      docf.reshape(blocks, BLOCK_LENGTH))


def mix_kernel(o_ref, qc_ref, cf_ref, cb_ref, doc_ref, edge_ref, gate_ref, gain_ref, out_ref):
    dk = cf_ref.shape[2]
    doc = doc_ref[...]
    qf = qc_ref[:, 0:dk]
    qb = qc_ref[:, dk : 2 * dk]
    total = o_ref[...]
    total = total + nt(qf, cf_ref[0]) * (doc == edge_ref[:, 0:1]).astype(F32)
    total = total + nt(qb, cb_ref[0]) * (doc == edge_ref[:, 1:2]).astype(F32)
    scaled = total * lax.rsqrt(jnp.mean(total * total, axis=-1, keepdims=True) + EPS)
    gate = gate_ref[...].astype(F32)
    act = gate / (1.0 + jnp.exp(-gate))
    out_ref[...] = (scaled * gain_ref[...].astype(F32) * act).astype(BF)


def head_mix(o, qc, cf, cb, docs, edges, gate, gain):
    rows = o.shape[0]
    heads, dv, dk = cf.shape
    tile = rows // 4
    per_head = pl.BlockSpec((1, dv, dk), lambda h, i: (h, 0, 0))
    return pl.pallas_call(
        mix_kernel,
        grid=(heads, 4),
        in_specs=[
            pl.BlockSpec((tile, dv), lambda h, i: (i, h)),
            pl.BlockSpec((tile, 2 * dk), lambda h, i: (i, h)),
            per_head, per_head,
            pl.BlockSpec((tile, 1), lambda h, i: (i, 0)),
            pl.BlockSpec((1, 2), lambda h, i: (0, 0)),
            pl.BlockSpec((tile, dv), lambda h, i: (i, h)),
            pl.BlockSpec((1, dv), lambda h, i: (0, 0)),
        ],
        out_specs=pl.BlockSpec((tile, dv), lambda h, i: (i, h)),
        out_shape=jax.ShapeDtypeStruct((rows, heads * dv), BF),
        cost_estimate=pl.CostEstimate(
            flops=5_000_000_000, bytes_accessed=12_000_000, transcendentals=0
        ),
        name="head_mix",
    )(o, qc, cf, cb, docs.astype(F32).reshape(rows, 1), edges, gate, gain.reshape(1, -1))


def shift(x, axis, by):
    n = lax.axis_size(axis)
    return lax.ppermute(x, axis, [(i, i + by) for i in range(n) if 0 <= i + by < n])


def rotate(x, axis, by):
    n = lax.axis_size(axis)
    return lax.ppermute(x, axis, [(i, (i + by) % n) for i in range(n)])


def carry_scan(states, decays, axis, signs):
    n = lax.axis_size(axis)

    def sent(s, a, by):
        return (shift(s.astype(BF), axis, by).astype(F32), shift(a, axis, by))

    pairs = [sent(s, a, g) for s, a, g in zip(states, decays, signs)]
    step = 1
    while step < n - 1:
        moved = [sent(s, a, g * step) for (s, a), g in zip(pairs, signs)]
        pairs = [(s + a * ms, a * ma) for (s, a), (ms, ma) in zip(pairs, moved)]
        step *= 2
    return [s.astype(BF) for s, _ in pairs]


def row_norm(rows_f, gain):
    factor = lax.rsqrt(jnp.mean(rows_f * rows_f, axis=-1, keepdims=True) + EPS)
    return (rows_f * factor * gain.astype(F32)).astype(BF)


def dot(a, b):
    return jnp.dot(a, b, preferred_element_type=F32)


def per_device(
    stream, queries, projected_keys, values, decay_gate_logits, decay_gate_bias,
    extra_log_decay, document_index, output_gate, head_norm_gain, output_weight,
    feedforward_norm_gain, gate_weight, up_weight, down_weight,
):
    gate_all = lax.all_gather(gate_weight, "sp", axis=0, tiled=True)
    up_all = lax.all_gather(up_weight, "sp", axis=0, tiled=True)
    down_all = lax.all_gather(down_weight, "sp", axis=1, tiled=True)
    docf = document_index.astype(F32)
    first, last = docf[:1], docf[-1:]
    prev_last = shift(last + 1.0, "sp", 1) - 1.0
    next_first = shift(first + 1.0, "sp", -1) - 1.0
    o, qc, sf, sb, logs = local_attention(
        queries, projected_keys, values, decay_gate_logits, decay_gate_bias,
        extra_log_decay, document_index,
    )
    decay = jnp.exp(logs)
    cf, cb = carry_scan(
        (sf, sb),
        (decay * (last == prev_last).astype(F32), decay * (first == next_first).astype(F32)),
        "sp",
        (1, -1),
    )
    edges = jnp.concatenate([prev_last, next_first]).reshape(1, 2)
    mixed = head_mix(o, qc, cf, cb, document_index, edges, output_gate, head_norm_gain)
    n = lax.axis_size("tp")
    me = lax.axis_index("tp")
    rows = stream.shape[0] // n

    def chunk(x, s):
        return lax.dynamic_slice_in_dim(x, (me + s) % n * rows, rows, 0)

    pieces = []
    for s in range(1, n):
        part = dot(chunk(mixed, s), output_weight).astype(BF)
        pieces.append(rotate(part, "tp", s))
    attended = dot(chunk(mixed, 0), output_weight).astype(BF).astype(F32)
    for piece in pieces:
        attended = attended + piece.astype(F32)
    resid = chunk(stream, 0).astype(F32) + attended
    normed = row_norm(resid, feedforward_norm_gain)
    others = [rotate(normed, "tp", s) for s in range(1, n)]

    def hidden_of(x):
        return (jax.nn.silu(dot(x, gate_all)) * dot(x, up_all)).astype(BF)

    own, *others = lax.optimization_barrier((hidden_of(normed), *others))
    parts = 2
    returned = []
    for s, x in enumerate(others, 1):
        hidden = hidden_of(x)
        cut = [
            rotate(dot(h, down_all).astype(BF), "tp", -s)
            for h in jnp.split(hidden, parts, axis=0)
        ]
        returned.append(cut)
    mlp_out = lax.optimization_barrier(dot(own, down_all).astype(BF)).astype(F32)
    for cut in returned:
        mlp_out = mlp_out + jnp.concatenate(cut, axis=0).astype(F32)
    return (resid + mlp_out).astype(BF)


def solution(mesh):
    placed = (
        P("sp", None), P("sp", "tp"), P("sp", "tp"), P("sp", "tp"), P("sp", "tp"), P("tp"),
        P("sp", "tp"), P("sp"), P("sp", "tp"), P(), P("tp", None), P(), P("sp", "tp"),
        P("sp", "tp"), P("tp", "sp"),
    )
    return jax.shard_map(
        per_device, mesh=mesh, in_specs=placed, out_specs=P(("sp", "tp"), None), check_vma=False
    )
```
